32 devices in a mesh: ep: 8 (over z, x), tp: 4 (over y, core).
Axes of the slice: x: 2, y: 2, z: 4, core: 2. Of those that a mesh axis runs over, the one named last changes fastest.
Arguments:
- queries: bfloat16 [1024, 4096], P('ep', 'tp'), may hold values from -112 to 112
- key_rows: bfloat16 [1024, 4096], P('ep', 'tp'), may hold values from -8.1 to 8.1
- values: bfloat16 [1024, 4096], P('ep', 'tp'), may hold values from -6 to 6
- lambdas: float32 [16], P('tp'), may hold values from 0.3 to 0.8
- head_gain: float32 [256], replicated, may hold values from 0.1 to 1.9
- tokens: bfloat16 [512, 4096], P('ep'), may hold values from -6 to 6
- moe_gain: float32 [4096], replicated, may hold values from 0.1 to 1.9
- routes: int32 [512, 2], P('ep'), may hold values from 0 to 7, all different within a row; in each aligned block of 64 rows (0 to 63, 64 to 127, ...) at most 32 rows name the same one
- route_scores: float32 [512, 2], P('ep'), may hold values from -6 to 6
- w_gate: bfloat16 [8, 4096, 2048], P('ep', None, 'tp'), may hold values from -0.09375 to 0.09375
- w_up: bfloat16 [8, 4096, 2048], P('ep', None, 'tp'), may hold values from -0.09375 to 0.09375
- w_down: bfloat16 [8, 2048, 4096], P('ep', 'tp'), may hold values from -0.125 to 0.125
Outputs:
- attended: bfloat16 [1024, 4096], P('ep', 'tp')
- expert_out: bfloat16 [512, 4096], P('ep', 'tp')
The draws below stay inside these ranges and needn't reach their ends.
Inputs may be any that keep to these rules, and one draw needn't show every extreme that they name: `routes`: each row names 2 different experts. Among the rows of one index of ep at most 32 name the same expert, and some index reaches 32 in every draw.
All inputs are finite; a program needn't handle non-finite values.
Results may differ from the reference program's by a relative error of at most 0.018.
Values may be sent and summed in bfloat16 or wider, within the bound.
A program may use at most 64 MiB of HBM per device.

```python
import math
from functools import partial
import jax
import jax.numpy as jnp
import numpy as np
from jax import lax

D = 4096
HEADS = 16
QKD = 128
VD = 256
FF = 2048
TOP = 2
TOKB_DEV = 64
SEQ = 1024
TOKB = 512
EXPERTS = 8
CAP = 32
N_EP = 8
N_TP = 4


def base_pairs(key):
    seed_one, seed_two, seed_three, seed_four, seed_five = jax.random.split(jax.random.fold_in(key, 11), 5)
    row_width = HEADS * 2 * QKD
    queries = jnp.clip(jax.random.normal(seed_one, (SEQ, row_width), jnp.float32) * 1.3, -8.0, 8.0)
    key_rows = jnp.clip(jax.random.normal(seed_two, (SEQ, row_width), jnp.float32) * 1.3, -8.0, 8.0)
    return (queries, key_rows, seed_three, seed_four, seed_five)


def draw_queries(key, part):
    drawn = base_pairs(key)
    return drawn[0].astype(jnp.bfloat16)


def draw_key_rows(key, part):
    drawn = base_pairs(key)
    return drawn[1].astype(jnp.bfloat16)


def block_levels(own_key, shape, cuts, smallest, largest):
    gain = 1.0
    for dim, parts in cuts:
        heights = jax.random.uniform(jax.random.fold_in(jax.random.fold_in(own_key, 6), dim), (parts,), jnp.float32, smallest / len(cuts), largest / len(cuts))
        gain = gain * jnp.repeat(jnp.exp(heights), shape[dim] // parts).reshape((-1,) + (1,) * (len(shape) - 1 - dim))
    return gain


def shared_out(rng, own, number, rows, amount, top, reach, lean):
    ranking = jax.random.permutation(rng, amount)
    heavy_load, usual = shares(amount, rows * top, reach, lean, True), shares(amount, rows * top, reach, lean, False)
    places = jnp.arange(amount)

    def named(tallies, offset_by):
        used = int((tallies > 0).sum())
        fixed = max(1, used // 4)
        passed = fixed + (places - fixed + offset_by * (used - fixed)) % max(1, amount - fixed)
        return jnp.zeros((amount,), jnp.int32).at[ranking[jnp.where(places < fixed, places, passed)]].set(jnp.asarray(tallies, jnp.int32))

    tallies = jnp.where(number % 4 == 0, named(heavy_load, number // 4), named(usual, number - number // 4 - 1))
    mixed = jax.random.permutation(jax.random.fold_in(own, 3), amount)
    giver, sink = mixed[0:amount // 2 * 2:2], mixed[1:amount // 2 * 2:2]
    margin = jnp.minimum(tallies[giver] - 1, reach - tallies[sink]) // 2
    margin = jnp.where((giver == ranking[0]) | (sink == ranking[0]) | (tallies[sink] == 0), 0, jnp.maximum(margin, 0))
    passed = jax.random.randint(jax.random.fold_in(own, 4), (amount // 2,), 0, 1 << 20) % (margin + 1)
    tallies = tallies.at[giver].add(-passed).at[sink].add(passed)
    members = jnp.searchsorted(jnp.cumsum(tallies), jnp.arange(rows * top), side="right").astype(jnp.int32)
    grid = members.reshape(top, rows).T
    grid = grid[jax.random.permutation(jax.random.fold_in(own, 1), rows)]
    offset_by = jax.random.randint(jax.random.fold_in(own, 2), (rows, 1), 0, top)
    return jnp.take_along_axis(grid, (jnp.arange(top)[None, :] + offset_by) % top, axis=1)


def shares(number_of, total, reach, slope, full):
    loads = [(1 << 20) // math.isqrt(standing ** slope) + 1 for standing in range(1, number_of + 1)]
    largest = reach if full else min(reach, max(-(-total // number_of), total * loads[0] // sum(loads)))
    least = 1 if total - largest >= number_of - 1 else 0
    given, spare = [largest] + [least] * (number_of - 1), total - largest - least * (number_of - 1)
    while spare > 0:
        candidates = [i for i in range(1, number_of) if given[i] < largest] or [i for i in range(1, number_of) if given[i] < reach]
        whole, budget = sum([loads[i] for i in candidates]), spare
        for i in candidates:
            extra = min(reach - given[i], max(1, budget * loads[i] // whole), spare)
            given[i] = given[i] + extra
            spare = spare - extra
    return np.array(given)


def bell_draw(own_key, dims, spread, limit, pieces=(), held_as=jnp.bfloat16):
    array = spread * jax.random.normal(own_key, dims, jnp.float32)
    if pieces:
        array = array * block_levels(own_key, dims, pieces, -0.22, 0.18)
    return jnp.clip(array, -limit, limit).astype(held_as)


def setup_inputs(seed: int = 0) -> dict:
    arg_keys = jax.random.split(jax.random.key(seed), 13)
    queries = draw_queries(jax.random.fold_in(arg_keys[12], 71), 0)
    key_rows = draw_key_rows(jax.random.fold_in(arg_keys[12], 71), 0)
    values = bell_draw(arg_keys[2], (SEQ, HEADS * VD), 1.0, 6.0, ((0, 8), (1, 4)))
    lambdas = jnp.clip(0.3 + 0.5 * jax.random.uniform(arg_keys[3], (HEADS,), jnp.float32) ** block_levels(arg_keys[3], (HEADS,), ((0, 4),), -0.2, 0.2), 0.3, 0.8)
    head_gain = jnp.clip(1.0 + 0.18 * jax.random.normal(arg_keys[4], (VD,), jnp.float32), 0.1, 1.9)
    tokens = bell_draw(arg_keys[5], (TOKB, D), 1.0, 6.0, ((0, 8),))
    moe_gain = jnp.clip(1.0 + 0.18 * jax.random.normal(arg_keys[6], (D,), jnp.float32), 0.1, 1.9)
    routes_keys = jax.random.split(jax.random.fold_in(arg_keys[7], 1), TOKB // TOKB_DEV)
    routes_turns = jax.random.permutation(jax.random.fold_in(arg_keys[7], 3), TOKB // TOKB_DEV)
    routes = jax.vmap(lambda own, number: shared_out(jax.random.fold_in(arg_keys[7], 2), own, number, TOKB_DEV, EXPERTS, TOP, CAP, 1))(routes_keys, routes_turns).reshape((TOKB, TOP))
    route_scores = bell_draw(arg_keys[8], (TOKB, TOP), 1.0, 6.0, ((0, 8),), jnp.float32)
    w_gate = bell_draw(arg_keys[9], (EXPERTS, D, FF), D ** -0.5, 0.09375, ((0, 8), (2, 4)))
    w_up = bell_draw(arg_keys[10], (EXPERTS, D, FF), D ** -0.5, 0.09375, ((0, 8), (2, 4)))
    w_down = bell_draw(arg_keys[11], (EXPERTS, FF, D), FF ** -0.5, 0.125, ((0, 8), (1, 4)))
    return {"queries": queries, "key_rows": key_rows, "values": values, "lambdas": lambdas, "head_gain": head_gain, "tokens": tokens, "moe_gain": moe_gain, "routes": routes, "route_scores": route_scores, "w_gate": w_gate, "w_up": w_up, "w_down": w_down}


neg_big = -1e+30
head_eps = 1e-05
moe_eps = 1e-06
head_scale = 0.8

def slot_table(routes, experts, capacity):
    flat_routes = routes.reshape(-1)
    onehot = (flat_routes[:, None] == jnp.arange(experts, dtype=jnp.int32)[None, :]).astype(jnp.int32)
    before = jnp.cumsum(onehot, axis=0) - onehot
    position = lax.optimization_barrier(jnp.sum(before * onehot, axis=1))
    return (flat_routes * capacity + position).astype(jnp.int32).reshape(routes.shape)

def reference(queries, key_rows, values, lambdas, head_gain, tokens, moe_gain, routes, route_scores, w_gate, w_up, w_down):
    query_heads = queries.reshape(SEQ, HEADS, 2, QKD).transpose(1, 0, 2, 3)
    key_heads = key_rows.reshape(SEQ, HEADS, 2, QKD).transpose(1, 0, 2, 3)
    value_heads = values.reshape(SEQ, HEADS, VD).transpose(1, 0, 2)
    visible = jnp.tril(jnp.ones((SEQ, SEQ), dtype=bool))

    def one_head(inputs):
        query_h, key_h, value_h, weight_h = inputs
        scores = jnp.einsum('qmd,kmd->mqk', query_h.astype(jnp.float32), key_h.astype(jnp.float32), precision=lax.Precision.HIGHEST) * QKD ** (-0.5)
        scores = jnp.where(visible[None], scores, neg_big)
        probabilities = jax.nn.softmax(scores, axis=-1)
        mixing = probabilities[0] - weight_h * probabilities[1]
        mixed_out = jnp.dot(mixing, value_h.astype(jnp.float32), precision=lax.Precision.HIGHEST)
        scaled = mixed_out * lax.rsqrt(lax.optimization_barrier(jnp.mean(mixed_out * mixed_out, axis=-1, keepdims=True)) + head_eps)
        return (scaled * head_gain * head_scale).astype(jnp.bfloat16)
    heads_out = lax.map(one_head, (query_heads, key_heads, value_heads, lambdas))
    attended = heads_out.transpose(1, 0, 2).reshape(SEQ, HEADS * VD)
    token_f32 = tokens.astype(jnp.float32)
    normed = (token_f32 * lax.rsqrt(lax.optimization_barrier(jnp.mean(token_f32 * token_f32, axis=-1, keepdims=True)) + moe_eps) * moe_gain).astype(jnp.bfloat16)
    gate_weights = jax.nn.softmax(route_scores, axis=-1)
    local_slots = jax.vmap(partial(slot_table, experts=EXPERTS, capacity=CAP))(routes.reshape(N_EP, TOKB_DEV, TOP))
    expert_ids = local_slots // CAP
    within = local_slots % CAP
    source = jnp.arange(N_EP, dtype=jnp.int32)[:, None, None]
    global_slot = (expert_ids * (N_EP * CAP) + source * CAP + within).astype(jnp.int32).reshape(TOKB, TOP)
    row_ids = jnp.broadcast_to(jnp.arange(TOKB, dtype=jnp.int32)[:, None], (TOKB, TOP))
    row_of_slot = jnp.zeros((EXPERTS * N_EP * CAP,), jnp.int32).at[global_slot.reshape(-1)].set(row_ids.reshape(-1))
    gathered = normed[row_of_slot].reshape(EXPERTS, N_EP * CAP, D)
    group_size = FF // N_TP

    def one_expert(inputs):
        rows_e, gate_e, up_e, down_e = inputs
        gate_act = jnp.dot(rows_e, gate_e, preferred_element_type=jnp.float32)
        up_act = jnp.dot(rows_e, up_e, preferred_element_type=jnp.float32)
        hidden = (jax.nn.silu(gate_act) * up_act).astype(jnp.bfloat16)

        def add_group(group_index, running):
            offset = (group_index * group_size).astype(jnp.int32)
            hidden_part = lax.dynamic_slice_in_dim(hidden, offset, group_size, 1)
            down_part = lax.dynamic_slice_in_dim(down_e, offset, group_size, 0)
            partial_sum = jnp.dot(hidden_part, down_part, preferred_element_type=jnp.float32).astype(jnp.bfloat16)
            partial_sum = lax.optimization_barrier(partial_sum)
            return running + partial_sum.astype(jnp.float32)
        running = lax.fori_loop(jnp.int32(0), jnp.int32(N_TP), add_group, jnp.zeros((N_EP * CAP, D), jnp.float32))
        return running.astype(jnp.bfloat16)
    results = lax.map(one_expert, (gathered, w_gate, w_up, w_down)).reshape(EXPERTS * N_EP * CAP, D)
    picked = results[global_slot].astype(jnp.float32)
    expert_out = lax.optimization_barrier(jnp.sum(gate_weights[..., None] * picked, axis=1)).astype(jnp.bfloat16)
    return (attended, expert_out)
```

```python
import functools

import jax
import jax.numpy as jnp
from jax import lax
from jax.experimental import pallas as pl
from jax.experimental.pallas import tpu as pltpu
from jax.sharding import PartitionSpec as P

QKD = 128
VD = 256
TOP = 2


neg_big = -1e30
head_eps = 1e-05
moe_eps = 1e-06
head_scale = 0.8


def slot_table(routes, experts, capacity):
    flat_routes = routes.reshape(-1)
    onehot = (flat_routes[:, None] == jnp.arange(experts, dtype=jnp.int32)[None, :]).astype(
        jnp.int32
    )
    before = jnp.cumsum(onehot, axis=0) - onehot
    position = jnp.sum(before * onehot, axis=1)
    return (flat_routes * capacity + position).reshape(routes.shape)


def fold_block(state, query_group, query_pos, key_heads, value_heads, key_pos):
    maxima, denominators, accumulated = state
    scores = jnp.einsum(
        "qhmd,khmd->hmqk", query_group, key_heads, preferred_element_type=jnp.float32
    ) * QKD ** (-0.5)
    visible = key_pos[None, :] <= query_pos[:, None]
    scores = jnp.where(visible, scores, neg_big)
    new_max = jnp.maximum(maxima, jnp.max(scores, axis=-1))
    weights = jnp.where(visible, jnp.exp(scores - new_max[..., None]), 0.0)
    accumulated = jnp.einsum(
        "hmqk,khd->hmqd", weights, value_heads, precision=lax.Precision.HIGHEST
    )
    denominators = jnp.sum(weights, axis=-1)
    return (new_max, denominators, accumulated)


def local_general(
    queries,
    key_rows,
    values,
    lambdas,
    head_gain,
    tokens,
    moe_gain,
    routes,
    route_scores,
    w_gate,
    w_up,
    w_down,
):
    rows_a = queries.shape[0]
    half_rows = rows_a // 2
    head_local = lambdas.shape[0]
    ep_count = lax.axis_size("ep")
    ep_index = lax.axis_index("ep")
    early_queries = queries[:half_rows]
    later_queries = queries[half_rows:]
    early_pos = ep_index * rows_a + jnp.arange(half_rows, dtype=jnp.int32)
    later_pos = ep_index * rows_a + half_rows + jnp.arange(half_rows, dtype=jnp.int32)
    query_groups = (
        early_queries.reshape(half_rows, head_local, 2, QKD),
        later_queries.reshape(half_rows, head_local, 2, QKD),
    )
    position_groups = (early_pos, later_pos)
    start_state = (
        jnp.full((head_local, 2, half_rows), neg_big, jnp.float32),
        jnp.zeros((head_local, 2, half_rows), jnp.float32),
        jnp.zeros((head_local, 2, half_rows, VD), jnp.float32),
    )
    totals = (start_state, start_state)
    row_start = jnp.int32(0)
    key_block = lax.all_gather(key_rows, "ep", axis=0, tiled=True)
    value_block = lax.all_gather(values, "ep", axis=0, tiled=True)
    key_count = key_block.shape[0]
    key_heads = key_block.reshape(key_count, head_local, 2, QKD)
    value_heads = value_block.reshape(key_count, head_local, VD).astype(jnp.float32)
    key_pos = jnp.arange(key_count, dtype=jnp.int32)
    updated = []
    for attend_group_index in range(2):
        state = totals[attend_group_index]
        query_group = query_groups[attend_group_index]
        query_pos = position_groups[attend_group_index]
        state = lax.cond(
            row_start <= query_pos[-1],
            lambda held: fold_block(held, query_group, query_pos, key_heads, value_heads, key_pos),
            lambda held: held,
            state,
        )
        updated.append(state)
    folded = (updated[0], updated[1])
    attended_groups = []
    for group_index in range(2):
        maxima, denominators, accumulated = folded[group_index]
        mixed_out = (
            accumulated[:, 0] / denominators[:, 0, :, None]
            - lambdas[:, None, None] * accumulated[:, 1] / denominators[:, 1, :, None]
        )
        scaled = mixed_out * lax.rsqrt(
            jnp.mean(mixed_out * mixed_out, axis=-1, keepdims=True) + head_eps
        )
        scaled = scaled * head_gain * head_scale
        attended_groups.append(
            scaled.transpose(1, 0, 2).reshape(half_rows, head_local * VD).astype(jnp.bfloat16)
        )
    later_out = attended_groups[1]
    attended = jnp.concatenate([attended_groups[0], later_out], axis=0)
    rows_b = tokens.shape[0]
    capacity = 2 * TOP * rows_b // ep_count
    token_f32 = tokens.astype(jnp.float32)
    normed = (
        token_f32
        * lax.rsqrt(jnp.mean(token_f32 * token_f32, axis=-1, keepdims=True) + moe_eps)
        * moe_gain
    ).astype(jnp.bfloat16)
    gate_weights = jax.nn.softmax(route_scores, axis=-1)
    slot_of = slot_table(routes, ep_count, capacity)
    row_ids = jnp.broadcast_to(jnp.arange(rows_b, dtype=jnp.int32)[:, None], slot_of.shape)
    row_of_slot = (
        jnp.zeros((ep_count * capacity,), jnp.int32)
        .at[slot_of.reshape(-1)]
        .set(row_ids.reshape(-1))
    )
    gate_local = w_gate[0]
    up_local = w_up[0]
    down_local = w_down[0]
    outgoing = normed[row_of_slot]
    arrived = lax.all_to_all(outgoing, "ep", split_axis=0, concat_axis=0, tiled=True)
    gate_act = jnp.dot(arrived, gate_local, preferred_element_type=jnp.float32)
    up_act = jnp.dot(arrived, up_local, preferred_element_type=jnp.float32)
    hidden = (jax.nn.silu(gate_act) * up_act).astype(jnp.bfloat16)
    summed = lax.psum_scatter(
        lax.dot_general(
            down_local, hidden, (((0,), (1,)), ((), ())), preferred_element_type=jnp.float32
        ).astype(jnp.bfloat16),
        "tp",
        scatter_dimension=0,
        tiled=True,
    )
    returned = lax.all_to_all(summed, "ep", split_axis=1, concat_axis=1, tiled=True)
    slot_ids = jnp.arange(ep_count * capacity, dtype=jnp.int32)
    combined = jnp.zeros((rows_b, returned.shape[0]), jnp.float32)
    for choice_index in range(TOP):
        picker = (slot_of[:, choice_index, None] == slot_ids[None, :]).astype(jnp.bfloat16)
        picked = lax.dot_general(
            picker, returned, (((1,), (1,)), ((), ())), preferred_element_type=jnp.float32
        )
        combined = combined + gate_weights[:, choice_index, None] * picked
    expert_out = combined.astype(jnp.bfloat16)
    return (attended, expert_out)


MESH = pl.DeviceIdType.MESH


def step_kernel(
    n,
    heads,
    q_ref,
    k_ref,
    v_ref,
    lam_ref,
    gain_ref,
    tok_ref,
    pick_ref,
    gate_ref,
    wg_ref,
    wu_ref,
    wd_ref,
    att_ref,
    out_ref,
    wg,
    wu,
    wd,
    qbuf,
    kbuf,
    vbuf,
    osend,
    oret,
    arr,
    part,
    near,
    csum,
    far,
    res,
    ret,
    w_sem,
    tok_send,
    tok_recv,
    ty_send,
    ty_recv,
    tc_send,
    tc_recv,
    a_send,
    a_recv,
    o_send,
    o_recv,
    rc_send,
    rc_recv,
    ry_send,
    ry_recv,
    e_send,
    e_recv,
):
    me = lax.axis_index("ep")
    tp = lax.axis_index("tp")
    y = tp // 2
    core = tp % 2
    tp_core = y * 2 + 1 - core
    tp_y = (1 - y) * 2 + core
    rows, slots, width = q_ref.shape[0], tok_ref.shape[1], tok_ref.shape[2]

    def peer(j):
        return lax.rem(me + j, n)

    def source(j):
        return lax.rem(me + n - j, n)

    def remote(src, dst, send, recv, ep, tpi):
        return pltpu.make_async_remote_copy(
            src_ref=src,
            dst_ref=dst,
            send_sem=send,
            recv_sem=recv,
            device_id=(ep, tpi),
            device_id_type=MESH,
        )

    loads = [
        pltpu.make_async_copy(wg_ref.at[0], wg, w_sem.at[0]),
        pltpu.make_async_copy(wu_ref.at[0], wu, w_sem.at[1]),
        pltpu.make_async_copy(wd_ref.at[0], wd, w_sem.at[2]),
    ]
    for load in loads:
        load.start()

    barrier = pltpu.get_barrier_semaphore()
    for j in range(1, n):
        pl.semaphore_signal(barrier, inc=1, device_id=(peer(j), tp), device_id_type=MESH)
    pl.semaphore_signal(barrier, inc=1, device_id=(me, tp_core), device_id_type=MESH)
    pl.semaphore_signal(barrier, inc=1, device_id=(me, tp_y), device_id_type=MESH)
    pl.semaphore_wait(barrier, n + 1)

    sent = []
    tok_copies = []
    for j in range(1, n):
        c = remote(
            tok_ref.at[peer(j)], arr.at[tp, me], tok_send.at[j], tok_recv.at[j], peer(j), tp
        )
        c.start()
        tok_copies.append(c)
    unit_copies = []
    for j in range(1, n):
        d = peer(j)
        cols = pl.ds(pl.multiple_of(d * QKD, QKD), QKD)
        vcols = pl.ds(pl.multiple_of((d // 2) * VD, VD), VD)
        group = [
            remote(q_ref.at[:, cols], qbuf.at[me], a_send.at[0, j], a_recv.at[0, j], d, tp),
            remote(k_ref.at[:, cols], kbuf.at[me], a_send.at[1, j], a_recv.at[1, j], d, tp),
            remote(v_ref.at[:, vcols], vbuf.at[me], a_send.at[2, j], a_recv.at[2, j], d, tp),
        ]
        for c in group:
            c.start()
        unit_copies.append(group)
    own = pl.ds(pl.multiple_of(me * QKD, QKD), QKD)
    own_v = pl.ds(pl.multiple_of((me // 2) * VD, VD), VD)
    qbuf[me] = q_ref[:, own]
    kbuf[me] = k_ref[:, own]
    vbuf[me] = v_ref[:, own_v]

    y_copies, core_copies = [], []
    for j in range(n):
        s = source(j)
        if j == 0:
            src = tok_ref.at[me]
            arr[tp, me] = tok_ref[me]
        else:
            tok_copies[j - 1].wait_recv()
            src = arr.at[tp, s]
        c = remote(src, arr.at[tp, s], ty_send.at[j], ty_recv.at[j], me, tp_y)
        c.start()
        y_copies.append(c)
        c = remote(src, arr.at[tp, s], tc_send.at[0, j], tc_recv.at[0, j], me, tp_core)
        c.start()
        core_copies.append(c)
    for j in range(n):
        s = source(j)
        y_copies[j].wait_recv()
        c = remote(
            arr.at[tp_y, s], arr.at[tp_y, s], tc_send.at[1, j], tc_recv.at[1, j], me, tp_core
        )
        c.start()
        core_copies.append(c)
    for c in core_copies:
        c.wait_recv()
    sent += tok_copies + y_copies + core_copies

    for load in loads:
        load.wait()
    total = n * slots
    gate = jnp.zeros((total, wg.shape[1]), jnp.float32)
    up = jnp.zeros((total, wg.shape[1]), jnp.float32)
    for i in range(4):
        a = arr[i].reshape(total, width)
        gate += jnp.dot(
            a, wg[i * width : (i + 1) * width, :], preferred_element_type=jnp.float32
        )
        up += jnp.dot(a, wu[i * width : (i + 1) * width, :], preferred_element_type=jnp.float32)
    hidden = (jax.nn.silu(gate) * up).astype(jnp.bfloat16)
    order = (tp_y + 1 - 2 * core, tp_y, tp_core, tp)
    near_copies = []
    for i in range(4):
        cols = pl.ds(pl.multiple_of(order[i] * width, width), width)
        part[i] = (
            jnp.dot(hidden, wd[:, cols], preferred_element_type=jnp.float32)
            .astype(jnp.bfloat16)
            .reshape(n, slots, width)
        )
        if i % 2 == 0:
            h = i // 2
            c = remote(part.at[i], near.at[h], rc_send.at[h], rc_recv.at[h], me, tp_core)
            c.start()
            near_copies.append(c)
    near_copies[0].wait_recv()
    far_copies = []
    for j in range(n):
        d = peer(j)
        csum[d] = (part[1, d].astype(jnp.float32) + near[0, d].astype(jnp.float32)).astype(
            jnp.bfloat16
        )
        c = remote(csum.at[d], far.at[d], ry_send.at[j], ry_recv.at[j], me, tp_y)
        c.start()
        far_copies.append(c)
    sent += near_copies + far_copies

    for group in unit_copies:
        for c in group:
            c.wait_recv()
        sent += group
    blk = 2
    size = blk * rows
    diag = (
        lax.broadcasted_iota(jnp.int32, (size, size), 1)
        <= lax.broadcasted_iota(jnp.int32, (size, size), 0)
    )
    for i in range(n // blk):
        seen = (i + 1) * size
        q = qbuf[i * blk : (i + 1) * blk].reshape(size, QKD)
        k = kbuf[0 : (i + 1) * blk].reshape(seen, QKD)
        v = vbuf[0 : (i + 1) * blk].reshape(seen, VD)
        scores = lax.dot_general(
            q, k, (((1,), (1,)), ((), ())), preferred_element_type=jnp.float32
        ) * QKD ** (-0.5)
        last = jnp.where(diag, scores[:, i * size :], neg_big)
        scores = last if i == 0 else jnp.concatenate([scores[:, : i * size], last], axis=1)
        weights = jnp.exp(scores - jnp.max(scores, axis=-1, keepdims=True))
        bottom = jnp.sum(weights, axis=-1, keepdims=True)
        o = jnp.dot(weights.astype(jnp.bfloat16), v, preferred_element_type=jnp.float32) / bottom
        osend[i * blk : (i + 1) * blk] = o.astype(jnp.bfloat16).reshape(blk, rows, VD)
        for s in range(i * blk, (i + 1) * blk):

            @pl.when(s != me)
            def _(s=s):
                remote(
                    osend.at[s], oret.at[me], o_send.at[s], o_recv.at[me], s, tp
                ).start()

    near_copies[1].wait_recv()
    back_copies = []
    for j in range(n):
        d = peer(j)
        far_copies[j].wait_recv()
        val = (
            part[3, d].astype(jnp.float32)
            + near[1, d].astype(jnp.float32)
            + far[d].astype(jnp.float32)
        ).astype(jnp.bfloat16)
        if j == 0:
            ret[me] = val
        else:
            res[d] = val
            c = remote(res.at[d], ret.at[me], e_send.at[j], e_recv.at[j], d, tp)
            c.start()
            back_copies.append(c)

    oret[me] = osend[me]
    for u in range(n):

        @pl.when(u != me)
        def _(u=u):
            remote(osend.at[u], oret.at[u], o_send.at[u], o_recv.at[u], u, tp).wait()

    for h in range(heads):
        mixed = oret[2 * h].astype(jnp.float32) - lam_ref[h] * oret[2 * h + 1].astype(jnp.float32)
        scaled = mixed * lax.rsqrt(jnp.mean(mixed * mixed, axis=-1, keepdims=True) + head_eps)
        att_ref[:, h * VD : (h + 1) * VD] = (scaled * gain_ref[...] * head_scale).astype(
            jnp.bfloat16
        )

    for c in back_copies:
        c.wait_recv()
    sent += back_copies
    returned = ret[...].reshape(total, width)
    combined = jnp.zeros(out_ref.shape, jnp.float32)
    for i in range(TOP):
        picked = jnp.dot(pick_ref[i], returned, preferred_element_type=jnp.float32)
        combined = combined + gate_ref[:, i : i + 1] * picked
    out_ref[...] = combined.astype(jnp.bfloat16)
    for c in sent:
        c.wait_send()


def local(
    queries,
    key_rows,
    values,
    lambdas,
    head_gain,
    tokens,
    moe_gain,
    routes,
    route_scores,
    w_gate,
    w_up,
    w_down,
):
    n = lax.axis_size("ep")
    heads = lambdas.shape[0]
    rows = queries.shape[0]
    rows_b, model = tokens.shape
    slots = 2 * TOP * rows_b // n
    width = model // 4
    ff = w_gate.shape[2]
    token_f32 = tokens.astype(jnp.float32)
    normed = (
        token_f32
        * lax.rsqrt(jnp.mean(token_f32 * token_f32, axis=-1, keepdims=True) + moe_eps)
        * moe_gain
    ).astype(jnp.bfloat16)
    gate_weights = jax.nn.softmax(route_scores, axis=-1)
    flat = routes.reshape(-1)
    count = flat.shape[0]
    place = jnp.arange(count, dtype=jnp.int32)
    earlier = (flat[:, None] == flat[None, :]) & (place[None, :] < place[:, None])
    slot_of = (flat * slots + jnp.sum(earlier.astype(jnp.int32), axis=1)).reshape(routes.shape)
    ids = jnp.arange(n * slots, dtype=jnp.int32)
    pick = (slot_of.T[:, :, None] == ids[None, None, :]).astype(jnp.bfloat16)
    mine = lax.dynamic_slice_in_dim(normed, lax.axis_index("tp") * width, width, 1)
    outgoing = (
        lax.dot_general(
            pick[0] + pick[1], mine, (((0,), (0,)), ((), ())), preferred_element_type=jnp.float32
        )
        .astype(jnp.bfloat16)
        .reshape(n, slots, width)
    )
    vmem = pl.BlockSpec(memory_space=pltpu.VMEM)
    hbm = pl.BlockSpec(memory_space=pl.ANY)
    smem = pl.BlockSpec(memory_space=pltpu.SMEM)
    bf16 = jnp.bfloat16
    dma = pltpu.SemaphoreType.DMA
    return tuple(
        pl.pallas_call(
            functools.partial(step_kernel, n, heads),
            out_shape=(
                jax.ShapeDtypeStruct(queries.shape, bf16),
                jax.ShapeDtypeStruct((rows_b, width), bf16),
            ),
            in_specs=[vmem, vmem, vmem, smem, vmem, vmem, vmem, vmem, hbm, hbm, hbm],
            out_specs=(vmem, vmem),
            scratch_shapes=[
                pltpu.VMEM((model, ff), bf16),
                pltpu.VMEM((model, ff), bf16),
                pltpu.VMEM((ff, model), bf16),
                pltpu.VMEM((n, rows, QKD), bf16),
                pltpu.VMEM((n, rows, QKD), bf16),
                pltpu.VMEM((n, rows, VD), bf16),
                pltpu.VMEM((n, rows, VD), bf16),
                pltpu.VMEM((n, rows, VD), bf16),
                pltpu.VMEM((4, n, slots, width), bf16),
                pltpu.VMEM((4, n, slots, width), bf16),
                pltpu.VMEM((2, n, slots, width), bf16),
                pltpu.VMEM((n, slots, width), bf16),
                pltpu.VMEM((n, slots, width), bf16),
                pltpu.VMEM((n, slots, width), bf16),
                pltpu.VMEM((n, slots, width), bf16),
                dma((3,)),
                dma((n,)),
                dma((n,)),
                dma((n,)),
                dma((n,)),
                dma((2, n)),
                dma((2, n)),
                dma((3, n)),
                dma((3, n)),
                dma((n,)),
                dma((n,)),
                dma((2,)),
                dma((2,)),
                dma((n,)),
                dma((n,)),
                dma((n,)),
                dma((n,)),
            ],
            compiler_params=pltpu.CompilerParams(
                collective_id=0, has_side_effects=True, vmem_limit_bytes=56 * 1024 * 1024
            ),
        )(
            queries,
            key_rows,
            values,
            lambdas,
            head_gain[None, :],
            outgoing,
            pick,
            gate_weights,
            w_gate,
            w_up,
            w_down,
        )
    )


def fits(mesh, head_count):
    n, parts = mesh.shape["ep"], mesh.shape["tp"]
    return parts == 4 and n % 2 == 0 and 2 * (head_count // parts) == n


def solution(mesh):
    def step(*args):
        body = local if fits(mesh, args[3].shape[0]) else local_general
        return sharded(mesh, body)(*args)

    return step


def sharded(mesh, body):
    return jax.shard_map(
        body,
        mesh=mesh,
        in_specs=(
            P("ep", "tp"),
            P("ep", "tp"),
            P("ep", "tp"),
            P("tp"),
            P(),
            P("ep", None),
            P(),
            P("ep", None),
            P("ep", None),
            P("ep", None, "tp"),
            P("ep", None, "tp"),
            P("ep", "tp", None),
        ),
        out_specs=(P("ep", "tp"), P("ep", "tp")),
        check_vma=False,
    )
```

```python
import functools

import jax
import jax.numpy as jnp
from jax import lax
from jax.experimental import pallas as pl
from jax.experimental.pallas import tpu as pltpu
from jax.sharding import PartitionSpec as P

QKD = 128
VD = 256
TOP = 2


neg_big = -1e30
head_eps = 1e-05
moe_eps = 1e-06
head_scale = 0.8


def slot_table(routes, experts, capacity):
    flat_routes = routes.reshape(-1)
    onehot = (flat_routes[:, None] == jnp.arange(experts, dtype=jnp.int32)[None, :]).astype(
        jnp.int32
    )
    before = jnp.cumsum(onehot, axis=0) - onehot
    position = jnp.sum(before * onehot, axis=1)
    return (flat_routes * capacity + position).reshape(routes.shape)


def fold_block(state, query_group, query_pos, key_heads, value_heads, key_pos):
    maxima, denominators, accumulated = state
    scores = jnp.einsum(
        "qhmd,khmd->hmqk", query_group, key_heads, preferred_element_type=jnp.float32
    ) * QKD ** (-0.5)
    visible = key_pos[None, :] <= query_pos[:, None]
    scores = jnp.where(visible, scores, neg_big)
    new_max = jnp.maximum(maxima, jnp.max(scores, axis=-1))
    weights = jnp.where(visible, jnp.exp(scores - new_max[..., None]), 0.0)
    accumulated = jnp.einsum(
        "hmqk,khd->hmqd", weights, value_heads, precision=lax.Precision.HIGHEST
    )
    denominators = jnp.sum(weights, axis=-1)
    return (new_max, denominators, accumulated)


def local_general(
    queries,
    key_rows,
    values,
    lambdas,
    head_gain,
    tokens,
    moe_gain,
    routes,
    route_scores,
    w_gate,
    w_up,
    w_down,
):
    rows_a = queries.shape[0]
    half_rows = rows_a // 2
    head_local = lambdas.shape[0]
    ep_count = lax.axis_size("ep")
    ep_index = lax.axis_index("ep")
    early_queries = queries[:half_rows]
    later_queries = queries[half_rows:]
    early_pos = ep_index * rows_a + jnp.arange(half_rows, dtype=jnp.int32)
    later_pos = ep_index * rows_a + half_rows + jnp.arange(half_rows, dtype=jnp.int32)
    query_groups = (
        early_queries.reshape(half_rows, head_local, 2, QKD),
        later_queries.reshape(half_rows, head_local, 2, QKD),
    )
    position_groups = (early_pos, later_pos)
    start_state = (
        jnp.full((head_local, 2, half_rows), neg_big, jnp.float32),
        jnp.zeros((head_local, 2, half_rows), jnp.float32),
        jnp.zeros((head_local, 2, half_rows, VD), jnp.float32),
    )
    totals = (start_state, start_state)
    row_start = jnp.int32(0)
    key_block = lax.all_gather(key_rows, "ep", axis=0, tiled=True)
    value_block = lax.all_gather(values, "ep", axis=0, tiled=True)
    key_count = key_block.shape[0]
    key_heads = key_block.reshape(key_count, head_local, 2, QKD)
    value_heads = value_block.reshape(key_count, head_local, VD).astype(jnp.float32)
    key_pos = jnp.arange(key_count, dtype=jnp.int32)
    updated = []
    for attend_group_index in range(2):
        state = totals[attend_group_index]
        query_group = query_groups[attend_group_index]
        query_pos = position_groups[attend_group_index]
        state = lax.cond(
            row_start <= query_pos[-1],
            lambda held: fold_block(held, query_group, query_pos, key_heads, value_heads, key_pos),
            lambda held: held,
            state,
        )
        updated.append(state)
    folded = (updated[0], updated[1])
    attended_groups = []
    for group_index in range(2):
        maxima, denominators, accumulated = folded[group_index]
        mixed_out = (
            accumulated[:, 0] / denominators[:, 0, :, None]
            - lambdas[:, None, None] * accumulated[:, 1] / denominators[:, 1, :, None]
        )
        scaled = mixed_out * lax.rsqrt(
            jnp.mean(mixed_out * mixed_out, axis=-1, keepdims=True) + head_eps
        )
        scaled = scaled * head_gain * head_scale
        attended_groups.append(
            scaled.transpose(1, 0, 2).reshape(half_rows, head_local * VD).astype(jnp.bfloat16)
        )
    later_out = attended_groups[1]
    attended = jnp.concatenate([attended_groups[0], later_out], axis=0)
    rows_b = tokens.shape[0]
    capacity = 2 * TOP * rows_b // ep_count
    token_f32 = tokens.astype(jnp.float32)
    normed = (
        token_f32
        * lax.rsqrt(jnp.mean(token_f32 * token_f32, axis=-1, keepdims=True) + moe_eps)
        * moe_gain
    ).astype(jnp.bfloat16)
    gate_weights = jax.nn.softmax(route_scores, axis=-1)
    slot_of = slot_table(routes, ep_count, capacity)
    row_ids = jnp.broadcast_to(jnp.arange(rows_b, dtype=jnp.int32)[:, None], slot_of.shape)
    row_of_slot = (
        jnp.zeros((ep_count * capacity,), jnp.int32)
        .at[slot_of.reshape(-1)]
        .set(row_ids.reshape(-1))
    )
    gate_local = w_gate[0]
    up_local = w_up[0]
    down_local = w_down[0]
    outgoing = normed[row_of_slot]
    arrived = lax.all_to_all(outgoing, "ep", split_axis=0, concat_axis=0, tiled=True)
    gate_act = jnp.dot(arrived, gate_local, preferred_element_type=jnp.float32)
    up_act = jnp.dot(arrived, up_local, preferred_element_type=jnp.float32)
    hidden = (jax.nn.silu(gate_act) * up_act).astype(jnp.bfloat16)
    summed = lax.psum_scatter(
        lax.dot_general(
            down_local, hidden, (((0,), (1,)), ((), ())), preferred_element_type=jnp.float32
        ).astype(jnp.bfloat16),
        "tp",
        scatter_dimension=0,
        tiled=True,
    )
    returned = lax.all_to_all(summed, "ep", split_axis=1, concat_axis=1, tiled=True)
    slot_ids = jnp.arange(ep_count * capacity, dtype=jnp.int32)
    combined = jnp.zeros((rows_b, returned.shape[0]), jnp.float32)
    for choice_index in range(TOP):
        picker = (slot_of[:, choice_index, None] == slot_ids[None, :]).astype(jnp.bfloat16)
        picked = lax.dot_general(
            picker, returned, (((1,), (1,)), ((), ())), preferred_element_type=jnp.float32
        )
        combined = combined + gate_weights[:, choice_index, None] * picked
    expert_out = combined.astype(jnp.bfloat16)
    return (attended, expert_out)


MESH = pl.DeviceIdType.MESH


def step_kernel(
    n,
    heads,
    q_ref,
    k_ref,
    v_ref,
    lam_ref,
    gain_ref,
    tokens_ref,
    moe_gain_ref,
    routes_ref,
    score_ref,
    wg_ref,
    wu_ref,
    wd_ref,
    att_ref,
    out_ref,
    wg,
    wu,
    wd,
    qbuf,
    kbuf,
    vbuf,
    osend,
    oret,
    fin,
    att_in,
    pick,
    tok,
    arr,
    part,
    near,
    csum,
    far,
    res,
    ret,
    w_sem,
    tok_send,
    tok_recv,
    ty_send,
    ty_recv,
    tc_send,
    tc_recv,
    a_send,
    a_recv,
    v_send,
    v_recv,
    o_send,
    o_recv,
    f_send,
    f_recv,
    rc_send,
    rc_recv,
    ry_send,
    ry_recv,
    e_send,
    e_recv,
):
    me = lax.axis_index("ep")
    tp = lax.axis_index("tp")
    y = tp // 2
    core = tp % 2
    tp_core = y * 2 + 1 - core
    tp_y = (1 - y) * 2 + core
    tp_both = (1 - y) * 2 + 1 - core
    side = me % 2
    head = me // 2
    pair = head * 2 + 1 - side
    rows = q_ref.shape[0]
    rows_b = tokens_ref.shape[0]
    _, slots, width = tok.shape
    total = n * slots

    def peer(j):
        return lax.rem(me + j, n)

    def source(j):
        return lax.rem(me + n - j, n)

    def remote(src, dst, send, recv, ep, tpi):
        return pltpu.make_async_remote_copy(
            src_ref=src,
            dst_ref=dst,
            send_sem=send,
            recv_sem=recv,
            device_id=(ep, tpi),
            device_id_type=MESH,
        )

    barrier = pltpu.get_barrier_semaphore()
    for j in range(1, n):
        pl.semaphore_signal(barrier, inc=1, device_id=(peer(j), tp), device_id_type=MESH)
    pl.semaphore_signal(barrier, inc=1, device_id=(me, tp_core), device_id_type=MESH)
    pl.semaphore_signal(barrier, inc=1, device_id=(me, tp_y), device_id_type=MESH)
    loads = [
        pltpu.make_async_copy(wg_ref.at[0], wg, w_sem.at[0]),
        pltpu.make_async_copy(wu_ref.at[0], wu, w_sem.at[1]),
        pltpu.make_async_copy(wd_ref.at[0], wd, w_sem.at[2]),
    ]
    for load in loads:
        load.start()

    features = pl.ds(pl.multiple_of(tp * width, width), width)
    token_f32 = tokens_ref[...].astype(jnp.float32)
    inverse = lax.rsqrt(jnp.mean(token_f32 * token_f32, axis=-1, keepdims=True) + moe_eps)
    normed = (
        tokens_ref[:, features].astype(jnp.float32) * inverse * moe_gain_ref[:, features]
    ).astype(jnp.bfloat16)
    lane = lax.broadcasted_iota(jnp.int32, (rows_b, 128), 1)
    named = [routes_ref[:, c : c + 1] == lane for c in range(TOP)]
    either = jnp.where(named[0] | named[1], 1.0, 0.0).astype(jnp.bfloat16)
    square = (rows_b, rows_b)
    below = jnp.where(
        lax.broadcasted_iota(jnp.int32, square, 1) < lax.broadcasted_iota(jnp.int32, square, 0),
        1.0,
        0.0,
    ).astype(jnp.bfloat16)
    before = jnp.dot(below, either, preferred_element_type=jnp.float32)
    slot_ids = lax.broadcasted_iota(jnp.int32, (rows_b, total), 1).astype(jnp.float32)
    chosen = jnp.zeros((rows_b, total), jnp.float32)
    for c in range(TOP):
        position = jnp.sum(jnp.where(named[c], before, 0.0), axis=1, keepdims=True)
        slot = routes_ref[:, c : c + 1].astype(jnp.float32) * slots + position
        hit = jnp.where(slot == slot_ids, 1.0, 0.0)
        pick[c] = hit.astype(jnp.bfloat16)
        chosen = chosen + hit
    tok[...] = (
        jnp.dot(chosen.T.astype(jnp.bfloat16), normed, preferred_element_type=jnp.float32)
        .astype(jnp.bfloat16)
        .reshape(n, slots, width)
    )
    pl.semaphore_wait(barrier, n + 1)

    sent = []
    tok_copies = []
    for j in range(1, n):
        c = remote(tok.at[peer(j)], arr.at[tp, me], tok_send.at[j], tok_recv.at[j], peer(j), tp)
        c.start()
        tok_copies.append(c)
    unit_copies = {}
    for which, src, dst in ((0, v_ref, None), (1, k_ref, kbuf.at[me]), (2, q_ref, qbuf.at[me])):
        for j in range(1, n):
            d = peer(j)
            cols = pl.ds(pl.multiple_of(d * QKD, QKD), QKD)
            to = vbuf.at[d % 2, me] if which == 0 else dst
            c = remote(src.at[:, cols], to, a_send.at[which, j], a_recv.at[which, j], d, tp)
            c.start()
            unit_copies[which, j] = c
    own = pl.ds(pl.multiple_of(me * QKD, QKD), QKD)
    qbuf[me] = q_ref[:, own]
    kbuf[me] = k_ref[:, own]
    vbuf[side, me] = v_ref[:, own]
    v_copies = [
        remote(v_ref.at[:, own], vbuf.at[side, me], v_send.at[me], v_recv.at[me], pair, tp)
    ]
    v_copies[0].start()

    y_copies, core_copies = [], ([], [])
    for j in range(n):
        s = source(j)
        if j == 0:
            src = tok.at[me]
            arr[tp, me] = tok[me]
        else:
            tok_copies[j - 1].wait_recv()
            src = arr.at[tp, s]
        c = remote(src, arr.at[tp, s], ty_send.at[j], ty_recv.at[j], me, tp_y)
        c.start()
        y_copies.append(c)
        c = remote(src, arr.at[tp, s], tc_send.at[0, j], tc_recv.at[0, j], me, tp_core)
        c.start()
        core_copies[0].append(c)

    def first_products(quarter):
        a = arr[quarter].reshape(total, width)
        deep = pl.ds(pl.multiple_of(quarter * width, width), width)
        return (
            jnp.dot(a, wg[deep, :], preferred_element_type=jnp.float32),
            jnp.dot(a, wu[deep, :], preferred_element_type=jnp.float32),
        )

    loads[0].wait()
    loads[1].wait()
    gate, up = first_products(tp)
    for c in core_copies[0]:
        c.wait_recv()
    more = first_products(tp_core)
    gate, up = gate + more[0], up + more[1]
    for j in range(n):
        s = source(j)
        y_copies[j].wait_recv()
        c = remote(
            arr.at[tp_y, s], arr.at[tp_y, s], tc_send.at[1, j], tc_recv.at[1, j], me, tp_core
        )
        c.start()
        core_copies[1].append(c)
    more = first_products(tp_y)
    gate, up = gate + more[0], up + more[1]
    for c in core_copies[1]:
        c.wait_recv()
    more = first_products(tp_both)
    gate, up = gate + more[0], up + more[1]
    sent += tok_copies + y_copies + core_copies[0] + core_copies[1]
    hidden = (jax.nn.silu(gate) * up).astype(jnp.bfloat16)

    loads[2].wait()
    order = (tp_both, tp_y, tp_core, tp)
    near_copies = []
    for i in range(4):
        cols = pl.ds(pl.multiple_of(order[i] * width, width), width)
        part[i] = (
            jnp.dot(hidden, wd[:, cols], preferred_element_type=jnp.float32)
            .astype(jnp.bfloat16)
            .reshape(n, slots, width)
        )
        if i % 2 == 0:
            h = i // 2
            c = remote(part.at[i], near.at[h], rc_send.at[h], rc_recv.at[h], me, tp_core)
            c.start()
            near_copies.append(c)
    near_copies[0].wait_recv()
    far_copies = []
    for j in range(n):
        d = peer(j)
        csum[d] = (part[1, d].astype(jnp.float32) + near[0, d].astype(jnp.float32)).astype(
            jnp.bfloat16
        )
        c = remote(csum.at[d], far.at[d], ry_send.at[j], ry_recv.at[j], me, tp_y)
        c.start()
        far_copies.append(c)
    sent += near_copies + far_copies
    near_copies[1].wait_recv()

    for j in range(1, n):
        s = source(j)
        unit_copies[0, j].wait_recv()
        c = remote(vbuf.at[side, s], vbuf.at[side, s], v_send.at[s], v_recv.at[s], pair, tp)
        c.start()
        v_copies.append(c)
    for j in range(1, n):
        unit_copies[1, j].wait_recv()
        unit_copies[2, j].wait_recv()
    for c in v_copies:
        c.wait_recv()
    sent += list(unit_copies.values()) + v_copies

    lam = lam_ref[head]
    keep = jnp.where(side == 0, 1.0, -lam)
    take = jnp.where(side == 0, -lam, 1.0)
    size = 2 * rows
    diag = (
        lax.broadcasted_iota(jnp.int32, (size, size), 1)
        <= lax.broadcasted_iota(jnp.int32, (size, size), 0)
    )
    back_copies = []

    def expert_back(j):
        d = peer(j)
        far_copies[j].wait_recv()
        val = (
            part[3, d].astype(jnp.float32)
            + near[1, d].astype(jnp.float32)
            + far[d].astype(jnp.float32)
        ).astype(jnp.bfloat16)
        if j == 0:
            ret[me] = val
        else:
            res[d] = val
            c = remote(res.at[d], ret.at[me], e_send.at[j], e_recv.at[j], d, tp)
            c.start()
            back_copies.append(c)

    swaps = []

    def finish(i):
        s = 2 * i + side
        swaps[i].wait_recv()
        mixed = keep * osend[s].astype(jnp.float32) + take * oret[i].astype(jnp.float32)
        scaled = mixed * lax.rsqrt(jnp.mean(mixed * mixed, axis=-1, keepdims=True) + head_eps)
        fin[i] = (scaled * gain_ref[...] * head_scale).astype(jnp.bfloat16)

        @pl.when(s != me)
        def _():
            remote(fin.at[i], att_in.at[head], f_send.at[i], f_recv.at[head], s, tp).start()

        @pl.when(s == me)
        def _():
            att_in[head] = fin[i]

    for i in range(n // 2):
        seen = (i + 1) * size
        q = qbuf[2 * i : 2 * i + 2].reshape(size, QKD)
        k = kbuf[0 : 2 * i + 2].reshape(seen, QKD)
        v = jnp.concatenate(
            [vbuf[half, 0 : 2 * i + 2].reshape(seen, VD // 2) for half in range(2)], axis=1
        )
        scores = lax.dot_general(
            q, k, (((1,), (1,)), ((), ())), preferred_element_type=jnp.float32
        ) * QKD ** (-0.5)
        last = jnp.where(diag, scores[:, i * size :], neg_big)
        scores = last if i == 0 else jnp.concatenate([scores[:, : i * size], last], axis=1)
        weights = jnp.exp(scores - jnp.max(scores, axis=-1, keepdims=True))
        bottom = jnp.sum(weights, axis=-1, keepdims=True)
        o = jnp.dot(weights.astype(jnp.bfloat16), v, preferred_element_type=jnp.float32) / bottom
        osend[2 * i : 2 * i + 2] = o.astype(jnp.bfloat16).reshape(2, rows, VD)
        c = remote(
            osend.at[2 * i + 1 - side], oret.at[i], o_send.at[i], o_recv.at[i], pair, tp
        )
        c.start()
        swaps.append(c)
        expert_back(2 * i)
        expert_back(2 * i + 1)
        if i > 0:
            finish(i - 1)
    finish(n // 2 - 1)
    sent += swaps + back_copies

    for h in range(heads):

        @pl.when(2 * h + side != me)
        def _(h=h):
            remote(
                fin.at[h], att_in.at[h], f_send.at[h], f_recv.at[h], 2 * h + side, tp
            ).wait()

        att_ref[:, h * VD : (h + 1) * VD] = att_in[h]

    for c in back_copies:
        c.wait_recv()
    first, second = score_ref[:, 0:1], score_ref[:, 1:2]
    top = jnp.maximum(first, second)
    raised = (jnp.exp(first - top), jnp.exp(second - top))
    returned = ret[...].reshape(total, width)
    combined = jnp.zeros(out_ref.shape, jnp.float32)
    for c in range(TOP):
        picked = jnp.dot(pick[c], returned, preferred_element_type=jnp.float32)
        combined = combined + raised[c] / (raised[0] + raised[1]) * picked
    out_ref[...] = combined.astype(jnp.bfloat16)
    for c in sent:
        c.wait_send()


def hand_over(att_ref, out_ref, att_to, out_to):
    att_to[...] = att_ref[...]
    out_to[...] = out_ref[...]


def local(
    queries,
    key_rows,
    values,
    lambdas,
    head_gain,
    tokens,
    moe_gain,
    routes,
    route_scores,
    w_gate,
    w_up,
    w_down,
):
    n = lax.axis_size("ep")
    heads = lambdas.shape[0]
    rows = queries.shape[0]
    rows_b, model = tokens.shape
    slots = 2 * TOP * rows_b // n
    width = model // 4
    ff = w_gate.shape[2]
    vmem = pl.BlockSpec(memory_space=pltpu.VMEM)
    hbm = pl.BlockSpec(memory_space=pl.ANY)
    smem = pl.BlockSpec(memory_space=pltpu.SMEM)
    bf16 = jnp.bfloat16
    dma = pltpu.SemaphoreType.DMA
    shapes = (
        jax.ShapeDtypeStruct(queries.shape, bf16),
        jax.ShapeDtypeStruct((rows_b, width), bf16),
    )
    held = pl.pallas_call(
        functools.partial(step_kernel, n, heads),
        out_shape=shapes,
        in_specs=[vmem, vmem, vmem, smem] + [vmem] * 5 + [hbm, hbm, hbm],
        out_specs=(vmem, vmem),
        scratch_shapes=[
            pltpu.VMEM((model, ff), bf16),
            pltpu.VMEM((model, ff), bf16),
            pltpu.VMEM((ff, model), bf16),
            pltpu.VMEM((n, rows, QKD), bf16),
            pltpu.VMEM((n, rows, QKD), bf16),
            pltpu.VMEM((2, n, rows, VD // 2), bf16),
            pltpu.VMEM((n, rows, VD), bf16),
            pltpu.VMEM((n // 2, rows, VD), bf16),
            pltpu.VMEM((n // 2, rows, VD), bf16),
            pltpu.VMEM((heads, rows, VD), bf16),
            pltpu.VMEM((TOP, rows_b, n * slots), bf16),
            pltpu.VMEM((n, slots, width), bf16),
            pltpu.VMEM((4, n, slots, width), bf16),
            pltpu.VMEM((4, n, slots, width), bf16),
            pltpu.VMEM((2, n, slots, width), bf16),
            pltpu.VMEM((n, slots, width), bf16),
            pltpu.VMEM((n, slots, width), bf16),
            pltpu.VMEM((n, slots, width), bf16),
            pltpu.VMEM((n, slots, width), bf16),
            dma((3,)),
            dma((n,)),
            dma((n,)),
            dma((n,)),
            dma((n,)),
            dma((2, n)),
            dma((2, n)),
            dma((3, n)),
            dma((3, n)),
            dma((n,)),
            dma((n,)),
            dma((n // 2,)),
            dma((n // 2,)),
            dma((n // 2,)),
            dma((n // 2,)),
            dma((2,)),
            dma((2,)),
            dma((n,)),
            dma((n,)),
            dma((n,)),
            dma((n,)),
        ],
        compiler_params=pltpu.CompilerParams(
            collective_id=0, has_side_effects=True, vmem_limit_bytes=56 * 1024 * 1024
        ),
    )(
        queries,
        key_rows,
        values,
        lambdas,
        head_gain[None, :],
        tokens,
        moe_gain[None, :],
        routes,
        route_scores,
        w_gate,
        w_up,
        w_down,
    )
    return tuple(
        pl.pallas_call(
            hand_over, out_shape=shapes, in_specs=[vmem, vmem], out_specs=(vmem, vmem)
        )(*held)
    )


def fits(mesh, head_count):
    n, parts = mesh.shape["ep"], mesh.shape["tp"]
    return parts == 4 and n % 2 == 0 and 2 * (head_count // parts) == n


def solution(mesh):
    def step(*args):
        body = local if fits(mesh, args[3].shape[0]) else local_general
        return sharded(mesh, body)(*args)

    return step


def sharded(mesh, body):
    return jax.shard_map(
        body,
        mesh=mesh,
        in_specs=(
            P("ep", "tp"),
            P("ep", "tp"),
            P("ep", "tp"),
            P("tp"),
            P(),
            P("ep", None),
            P(),
            P("ep", None),
            P("ep", None),
            P("ep", None, "tp"),
            P("ep", None, "tp"),
            P("ep", "tp", None),
        ),
        out_specs=(P("ep", "tp"), P("ep", "tp")),
        check_vma=False,
    )
```

```python
import functools

import jax
import jax.numpy as jnp
from jax import lax
from jax.experimental import pallas as pl
from jax.experimental.pallas import tpu as pltpu
from jax.sharding import PartitionSpec as P

QKD = 128
VD = 256
TOP = 2


neg_big = -1e30
head_eps = 1e-05
moe_eps = 1e-06
head_scale = 0.8


def slot_table(routes, experts, capacity):
    flat_routes = routes.reshape(-1)
    onehot = (flat_routes[:, None] == jnp.arange(experts, dtype=jnp.int32)[None, :]).astype(
        jnp.int32
    )
    before = jnp.cumsum(onehot, axis=0) - onehot
    position = jnp.sum(before * onehot, axis=1)
    return (flat_routes * capacity + position).reshape(routes.shape)


def fold_block(state, query_group, query_pos, key_heads, value_heads, key_pos):
    maxima, denominators, accumulated = state
    scores = jnp.einsum(
        "qhmd,khmd->hmqk", query_group, key_heads, preferred_element_type=jnp.float32
    ) * QKD ** (-0.5)
    visible = key_pos[None, :] <= query_pos[:, None]
    scores = jnp.where(visible, scores, neg_big)
    new_max = jnp.maximum(maxima, jnp.max(scores, axis=-1))
    weights = jnp.where(visible, jnp.exp(scores - new_max[..., None]), 0.0)
    accumulated = jnp.einsum(
        "hmqk,khd->hmqd", weights, value_heads, precision=lax.Precision.HIGHEST
    )
    denominators = jnp.sum(weights, axis=-1)
    return (new_max, denominators, accumulated)


def local_general(
    queries,
    key_rows,
    values,
    lambdas,
    head_gain,
    tokens,
    moe_gain,
    routes,
    route_scores,
    w_gate,
    w_up,
    w_down,
):
    rows_a = queries.shape[0]
    half_rows = rows_a // 2
    head_local = lambdas.shape[0]
    ep_count = lax.axis_size("ep")
    ep_index = lax.axis_index("ep")
    early_queries = queries[:half_rows]
    later_queries = queries[half_rows:]
    early_pos = ep_index * rows_a + jnp.arange(half_rows, dtype=jnp.int32)
    later_pos = ep_index * rows_a + half_rows + jnp.arange(half_rows, dtype=jnp.int32)
    query_groups = (
        early_queries.reshape(half_rows, head_local, 2, QKD),
        later_queries.reshape(half_rows, head_local, 2, QKD),
    )
    position_groups = (early_pos, later_pos)
    start_state = (
        jnp.full((head_local, 2, half_rows), neg_big, jnp.float32),
        jnp.zeros((head_local, 2, half_rows), jnp.float32),
        jnp.zeros((head_local, 2, half_rows, VD), jnp.float32),
    )
    totals = (start_state, start_state)
    row_start = jnp.int32(0)
    key_block = lax.all_gather(key_rows, "ep", axis=0, tiled=True)
    value_block = lax.all_gather(values, "ep", axis=0, tiled=True)
    key_count = key_block.shape[0]
    key_heads = key_block.reshape(key_count, head_local, 2, QKD)
    value_heads = value_block.reshape(key_count, head_local, VD).astype(jnp.float32)
    key_pos = jnp.arange(key_count, dtype=jnp.int32)
    updated = []
    for attend_group_index in range(2):
        state = totals[attend_group_index]
        query_group = query_groups[attend_group_index]
        query_pos = position_groups[attend_group_index]
        state = lax.cond(
            row_start <= query_pos[-1],
            lambda held: fold_block(held, query_group, query_pos, key_heads, value_heads, key_pos),
            lambda held: held,
            state,
        )
        updated.append(state)
    folded = (updated[0], updated[1])
    attended_groups = []
    for group_index in range(2):
        maxima, denominators, accumulated = folded[group_index]
        mixed_out = (
            accumulated[:, 0] / denominators[:, 0, :, None]
            - lambdas[:, None, None] * accumulated[:, 1] / denominators[:, 1, :, None]
        )
        scaled = mixed_out * lax.rsqrt(
            jnp.mean(mixed_out * mixed_out, axis=-1, keepdims=True) + head_eps
        )
        scaled = scaled * head_gain * head_scale
        attended_groups.append(
            scaled.transpose(1, 0, 2).reshape(half_rows, head_local * VD).astype(jnp.bfloat16)
        )
    later_out = attended_groups[1]
    attended = jnp.concatenate([attended_groups[0], later_out], axis=0)
    rows_b = tokens.shape[0]
    capacity = 2 * TOP * rows_b // ep_count
    token_f32 = tokens.astype(jnp.float32)
    normed = (
        token_f32
        * lax.rsqrt(jnp.mean(token_f32 * token_f32, axis=-1, keepdims=True) + moe_eps)
        * moe_gain
    ).astype(jnp.bfloat16)
    gate_weights = jax.nn.softmax(route_scores, axis=-1)
    slot_of = slot_table(routes, ep_count, capacity)
    row_ids = jnp.broadcast_to(jnp.arange(rows_b, dtype=jnp.int32)[:, None], slot_of.shape)
    row_of_slot = (
        jnp.zeros((ep_count * capacity,), jnp.int32)
        .at[slot_of.reshape(-1)]
        .set(row_ids.reshape(-1))
    )
    gate_local = w_gate[0]
    up_local = w_up[0]
    down_local = w_down[0]
    outgoing = normed[row_of_slot]
    arrived = lax.all_to_all(outgoing, "ep", split_axis=0, concat_axis=0, tiled=True)
    gate_act = jnp.dot(arrived, gate_local, preferred_element_type=jnp.float32)
    up_act = jnp.dot(arrived, up_local, preferred_element_type=jnp.float32)
    hidden = (jax.nn.silu(gate_act) * up_act).astype(jnp.bfloat16)
    summed = lax.psum_scatter(
        lax.dot_general(
            down_local, hidden, (((0,), (1,)), ((), ())), preferred_element_type=jnp.float32
        ).astype(jnp.bfloat16),
        "tp",
        scatter_dimension=0,
        tiled=True,
    )
    returned = lax.all_to_all(summed, "ep", split_axis=1, concat_axis=1, tiled=True)
    slot_ids = jnp.arange(ep_count * capacity, dtype=jnp.int32)
    combined = jnp.zeros((rows_b, returned.shape[0]), jnp.float32)
    for choice_index in range(TOP):
        picker = (slot_of[:, choice_index, None] == slot_ids[None, :]).astype(jnp.bfloat16)
        picked = lax.dot_general(
            picker, returned, (((1,), (1,)), ((), ())), preferred_element_type=jnp.float32
        )
        combined = combined + gate_weights[:, choice_index, None] * picked
    expert_out = combined.astype(jnp.bfloat16)
    return (attended, expert_out)


MESH = pl.DeviceIdType.MESH


def step_kernel(
    n,
    heads,
    q_ref,
    k_ref,
    v_ref,
    lam_ref,
    gain_ref,
    tokens_ref,
    moe_gain_ref,
    routes_ref,
    score_ref,
    wg_ref,
    wu_ref,
    wd_ref,
    att_ref,
    out_ref,
    wg,
    wu,
    wd,
    qbuf,
    kbuf,
    vbuf,
    osend,
    oret,
    fin,
    att_in,
    pick,
    tok,
    arr,
    part,
    near,
    csum,
    far,
    res,
    ret,
    w_sem,
    tok_send,
    tok_recv,
    ty_send,
    ty_recv,
    tc_send,
    tc_recv,
    a_send,
    a_recv,
    v_send,
    v_recv,
    o_send,
    o_recv,
    f_send,
    f_recv,
    rc_send,
    rc_recv,
    ry_send,
    ry_recv,
    e_send,
    e_recv,
):
    me = lax.axis_index("ep")
    tp = lax.axis_index("tp")
    y = tp // 2
    core = tp % 2
    tp_core = y * 2 + 1 - core
    tp_y = (1 - y) * 2 + core
    tp_both = (1 - y) * 2 + 1 - core
    side = me % 2
    head = me // 2
    pair = head * 2 + 1 - side
    rows = q_ref.shape[0]
    rows_b = tokens_ref.shape[0]
    _, slots, width = tok.shape
    total = n * slots

    def peer(j):
        return lax.rem(me + j, n)

    def source(j):
        return lax.rem(me + n - j, n)

    def remote(src, dst, send, recv, ep, tpi):
        return pltpu.make_async_remote_copy(
            src_ref=src,
            dst_ref=dst,
            send_sem=send,
            recv_sem=recv,
            device_id=(ep, tpi),
            device_id_type=MESH,
        )

    barrier = pltpu.get_barrier_semaphore()
    for j in range(1, n):
        pl.semaphore_signal(barrier, inc=1, device_id=(peer(j), tp), device_id_type=MESH)
    pl.semaphore_signal(barrier, inc=1, device_id=(me, tp_core), device_id_type=MESH)
    pl.semaphore_signal(barrier, inc=1, device_id=(me, tp_y), device_id_type=MESH)
    loads = [
        pltpu.make_async_copy(wg_ref.at[0], wg, w_sem.at[0]),
        pltpu.make_async_copy(wu_ref.at[0], wu, w_sem.at[1]),
        pltpu.make_async_copy(wd_ref.at[0], wd, w_sem.at[2]),
    ]
    for load in loads:
        load.start()

    features = pl.ds(pl.multiple_of(tp * width, width), width)
    token_f32 = tokens_ref[...].astype(jnp.float32)
    inverse = lax.rsqrt(jnp.mean(token_f32 * token_f32, axis=-1, keepdims=True) + moe_eps)
    normed = (
        tokens_ref[:, features].astype(jnp.float32) * inverse * moe_gain_ref[:, features]
    ).astype(jnp.bfloat16)
    lane = lax.broadcasted_iota(jnp.int32, (rows_b, 128), 1)
    square = (rows_b, rows_b)
    row_at = lax.broadcasted_iota(jnp.int32, square, 0)
    column_at = lax.broadcasted_iota(jnp.int32, square, 1)

    def upright(ref, c):
        line = jnp.broadcast_to(ref[c : c + 1, :], square)
        return jnp.sum(
            jnp.where(row_at == column_at, line, jnp.zeros_like(line)), axis=1, keepdims=True
        )

    named_by = [upright(routes_ref, c) for c in range(TOP)]
    named = [named_by[c] == lane for c in range(TOP)]
    either = jnp.where(named[0] | named[1], 1.0, 0.0).astype(jnp.bfloat16)
    below = jnp.where(column_at < row_at, 1.0, 0.0).astype(jnp.bfloat16)
    before = jnp.dot(below, either, preferred_element_type=jnp.float32)
    slot_ids = lax.broadcasted_iota(jnp.int32, (rows_b, total), 1).astype(jnp.float32)
    chosen = jnp.zeros((rows_b, total), jnp.float32)
    for c in range(TOP):
        position = jnp.sum(jnp.where(named[c], before, 0.0), axis=1, keepdims=True)
        slot = named_by[c].astype(jnp.float32) * slots + position
        hit = jnp.where(slot == slot_ids, 1.0, 0.0)
        pick[c] = hit.astype(jnp.bfloat16)
        chosen = chosen + hit
    tok[...] = (
        jnp.dot(chosen.T.astype(jnp.bfloat16), normed, preferred_element_type=jnp.float32)
        .astype(jnp.bfloat16)
        .reshape(n, slots, width)
    )
    pl.semaphore_wait(barrier, n + 1)

    sent = []
    tok_copies = []
    for j in range(1, n):
        c = remote(tok.at[peer(j)], arr.at[tp, me], tok_send.at[j], tok_recv.at[j], peer(j), tp)
        c.start()
        tok_copies.append(c)
    unit_copies = {}
    for which, src, dst in ((0, v_ref, None), (1, k_ref, kbuf.at[me]), (2, q_ref, qbuf.at[me])):
        for j in range(1, n):
            d = peer(j)
            cols = pl.ds(pl.multiple_of(d * QKD, QKD), QKD)
            to = vbuf.at[d % 2, me] if which == 0 else dst
            c = remote(src.at[:, cols], to, a_send.at[which, j], a_recv.at[which, j], d, tp)
            c.start()
            unit_copies[which, j] = c
    own = pl.ds(pl.multiple_of(me * QKD, QKD), QKD)
    qbuf[me] = q_ref[:, own]
    kbuf[me] = k_ref[:, own]
    vbuf[side, me] = v_ref[:, own]
    v_copies = [
        remote(v_ref.at[:, own], vbuf.at[side, me], v_send.at[me], v_recv.at[me], pair, tp)
    ]
    v_copies[0].start()

    y_copies, core_copies = [], ([], [])
    for j in range(n):
        s = source(j)
        if j == 0:
            src = tok.at[me]
            arr[tp, me] = tok[me]
        else:
            tok_copies[j - 1].wait_recv()
            src = arr.at[tp, s]
        c = remote(src, arr.at[tp, s], ty_send.at[j], ty_recv.at[j], me, tp_y)
        c.start()
        y_copies.append(c)
        c = remote(src, arr.at[tp, s], tc_send.at[0, j], tc_recv.at[0, j], me, tp_core)
        c.start()
        core_copies[0].append(c)

    def first_products(quarter):
        a = arr[quarter].reshape(total, width)
        deep = pl.ds(pl.multiple_of(quarter * width, width), width)
        return (
            jnp.dot(a, wg[deep, :], preferred_element_type=jnp.float32),
            jnp.dot(a, wu[deep, :], preferred_element_type=jnp.float32),
        )

    loads[0].wait()
    loads[1].wait()
    gate, up = first_products(tp)
    for c in core_copies[0]:
        c.wait_recv()
    more = first_products(tp_core)
    gate, up = gate + more[0], up + more[1]
    for j in range(n):
        s = source(j)
        y_copies[j].wait_recv()
        c = remote(
            arr.at[tp_y, s], arr.at[tp_y, s], tc_send.at[1, j], tc_recv.at[1, j], me, tp_core
        )
        c.start()
        core_copies[1].append(c)
    more = first_products(tp_y)
    gate, up = gate + more[0], up + more[1]
    for c in core_copies[1]:
        c.wait_recv()
    more = first_products(tp_both)
    gate, up = gate + more[0], up + more[1]
    sent += tok_copies + y_copies + core_copies[0] + core_copies[1]
    for j in range(1, n):
        s = source(j)
        unit_copies[0, j].wait_recv()
        c = remote(vbuf.at[side, s], vbuf.at[side, s], v_send.at[s], v_recv.at[s], pair, tp)
        c.start()
        v_copies.append(c)
    hidden = (jax.nn.silu(gate) * up).astype(jnp.bfloat16)

    loads[2].wait()
    order = (tp_both, tp_y, tp_core, tp)
    near_copies = []
    for i in range(4):
        cols = pl.ds(pl.multiple_of(order[i] * width, width), width)
        part[i] = (
            jnp.dot(hidden, wd[:, cols], preferred_element_type=jnp.float32)
            .astype(jnp.bfloat16)
            .reshape(n, slots, width)
        )
        if i % 2 == 0:
            h = i // 2
            c = remote(part.at[i], near.at[h], rc_send.at[h], rc_recv.at[h], me, tp_core)
            c.start()
            near_copies.append(c)
    near_copies[0].wait_recv()
    far_copies = []
    for j in range(n):
        d = peer(j)
        csum[d] = (part[1, d].astype(jnp.float32) + near[0, d].astype(jnp.float32)).astype(
            jnp.bfloat16
        )
        c = remote(csum.at[d], far.at[d], ry_send.at[j], ry_recv.at[j], me, tp_y)
        c.start()
        far_copies.append(c)
    sent += near_copies + far_copies
    near_copies[1].wait_recv()

    for j in range(1, n):
        unit_copies[1, j].wait_recv()
        unit_copies[2, j].wait_recv()
    for c in v_copies:
        c.wait_recv()
    sent += list(unit_copies.values()) + v_copies

    lam = lam_ref[head]
    keep = jnp.where(side == 0, 1.0, -lam)
    take = jnp.where(side == 0, -lam, 1.0)
    size = 2 * rows
    diag = (
        lax.broadcasted_iota(jnp.int32, (size, size), 1)
        <= lax.broadcasted_iota(jnp.int32, (size, size), 0)
    )
    back_copies = []

    def expert_back(j):
        d = peer(j)
        far_copies[j].wait_recv()
        val = (
            part[3, d].astype(jnp.float32)
            + near[1, d].astype(jnp.float32)
            + far[d].astype(jnp.float32)
        ).astype(jnp.bfloat16)
        if j == 0:
            ret[me] = val
        else:
            res[d] = val
            c = remote(res.at[d], ret.at[me], e_send.at[j], e_recv.at[j], d, tp)
            c.start()
            back_copies.append(c)

    swaps = []

    def finish(i):
        s = 2 * i + side
        swaps[i].wait_recv()
        mixed = keep * osend[s].astype(jnp.float32) + take * oret[i].astype(jnp.float32)
        scaled = mixed * lax.rsqrt(jnp.mean(mixed * mixed, axis=-1, keepdims=True) + head_eps)
        fin[i] = (scaled * gain_ref[...] * head_scale).astype(jnp.bfloat16)

        @pl.when(s != me)
        def _():
            remote(fin.at[i], att_in.at[head], f_send.at[i], f_recv.at[head], s, tp).start()

        @pl.when(s == me)
        def _():
            att_in[head] = fin[i]

    for i in range(n // 2):
        seen = (i + 1) * size
        q = qbuf[2 * i : 2 * i + 2].reshape(size, QKD)
        k = kbuf[0 : 2 * i + 2].reshape(seen, QKD)
        v = jnp.concatenate(
            [vbuf[half, 0 : 2 * i + 2].reshape(seen, VD // 2) for half in range(2)], axis=1
        )
        scores = lax.dot_general(
            q, k, (((1,), (1,)), ((), ())), preferred_element_type=jnp.float32
        ) * QKD ** (-0.5)
        last = jnp.where(diag, scores[:, i * size :], neg_big)
        scores = last if i == 0 else jnp.concatenate([scores[:, : i * size], last], axis=1)
        weights = jnp.exp(scores - jnp.max(scores, axis=-1, keepdims=True))
        bottom = jnp.sum(weights, axis=-1, keepdims=True)
        o = jnp.dot(weights.astype(jnp.bfloat16), v, preferred_element_type=jnp.float32) / bottom
        osend[2 * i : 2 * i + 2] = o.astype(jnp.bfloat16).reshape(2, rows, VD)
        c = remote(
            osend.at[2 * i + 1 - side], oret.at[i], o_send.at[i], o_recv.at[i], pair, tp
        )
        c.start()
        swaps.append(c)
        expert_back(2 * i)
        expert_back(2 * i + 1)
        if i > 0:
            finish(i - 1)
    finish(n // 2 - 1)
    sent += swaps + back_copies

    for h in range(heads):

        @pl.when(2 * h + side != me)
        def _(h=h):
            remote(
                fin.at[h], att_in.at[h], f_send.at[h], f_recv.at[h], 2 * h + side, tp
            ).wait()

        att_ref[:, h * VD : (h + 1) * VD] = att_in[h]

    for c in back_copies:
        c.wait_recv()
    first, second = upright(score_ref, 0), upright(score_ref, 1)
    top = jnp.maximum(first, second)
    raised = (jnp.exp(first - top), jnp.exp(second - top))
    returned = ret[...].reshape(total, width)
    combined = jnp.zeros(out_ref.shape, jnp.float32)
    for c in range(TOP):
        picked = jnp.dot(pick[c], returned, preferred_element_type=jnp.float32)
        combined = combined + raised[c] / (raised[0] + raised[1]) * picked
    out_ref[...] = combined.astype(jnp.bfloat16)
    for c in sent:
        c.wait_send()


def hand_over(att_ref, out_ref, att_to, out_to):
    att_to[...] = att_ref[...]
    out_to[...] = out_ref[...]


def local(
    queries,
    key_rows,
    values,
    lambdas,
    head_gain,
    tokens,
    moe_gain,
    routes,
    route_scores,
    w_gate,
    w_up,
    w_down,
):
    n = lax.axis_size("ep")
    heads = lambdas.shape[0]
    rows = queries.shape[0]
    rows_b, model = tokens.shape
    slots = 2 * TOP * rows_b // n
    width = model // 4
    ff = w_gate.shape[2]
    vmem = pl.BlockSpec(memory_space=pltpu.VMEM)
    hbm = pl.BlockSpec(memory_space=pl.ANY)
    smem = pl.BlockSpec(memory_space=pltpu.SMEM)
    bf16 = jnp.bfloat16
    dma = pltpu.SemaphoreType.DMA
    shapes = (
        jax.ShapeDtypeStruct(queries.shape, bf16),
        jax.ShapeDtypeStruct((rows_b, width), bf16),
    )
    held = pl.pallas_call(
        functools.partial(step_kernel, n, heads),
        out_shape=shapes,
        in_specs=[vmem, vmem, vmem, smem] + [vmem] * 5 + [hbm, hbm, hbm],
        out_specs=(vmem, vmem),
        scratch_shapes=[
            pltpu.VMEM((model, ff), bf16),
            pltpu.VMEM((model, ff), bf16),
            pltpu.VMEM((ff, model), bf16),
            pltpu.VMEM((n, rows, QKD), bf16),
            pltpu.VMEM((n, rows, QKD), bf16),
            pltpu.VMEM((2, n, rows, VD // 2), bf16),
            pltpu.VMEM((n, rows, VD), bf16),
            pltpu.VMEM((n // 2, rows, VD), bf16),
            pltpu.VMEM((n // 2, rows, VD), bf16),
            pltpu.VMEM((heads, rows, VD), bf16),
            pltpu.VMEM((TOP, rows_b, n * slots), bf16),
            pltpu.VMEM((n, slots, width), bf16),
            pltpu.VMEM((4, n, slots, width), bf16),
            pltpu.VMEM((4, n, slots, width), bf16),
            pltpu.VMEM((2, n, slots, width), bf16),
            pltpu.VMEM((n, slots, width), bf16),
            pltpu.VMEM((n, slots, width), bf16),
            pltpu.VMEM((n, slots, width), bf16),
            pltpu.VMEM((n, slots, width), bf16),
            dma((3,)),
            dma((n,)),
            dma((n,)),
            dma((n,)),
            dma((n,)),
            dma((2, n)),
            dma((2, n)),
            dma((3, n)),
            dma((3, n)),
            dma((n,)),
            dma((n,)),
            dma((n // 2,)),
            dma((n // 2,)),
            dma((n // 2,)),
            dma((n // 2,)),
            dma((2,)),
            dma((2,)),
            dma((n,)),
            dma((n,)),
            dma((n,)),
            dma((n,)),
        ],
        compiler_params=pltpu.CompilerParams(
            collective_id=0, has_side_effects=True, vmem_limit_bytes=56 * 1024 * 1024
        ),
    )(
        queries,
        key_rows,
        values,
        lambdas,
        head_gain[None, :],
        tokens,
        moe_gain[None, :],
        routes.T,
        route_scores.T,
        w_gate,
        w_up,
        w_down,
    )
    return tuple(
        pl.pallas_call(
            hand_over, out_shape=shapes, in_specs=[vmem, vmem], out_specs=(vmem, vmem)
        )(*held)
    )


def fits(mesh, head_count):
    n, parts = mesh.shape["ep"], mesh.shape["tp"]
    return parts == 4 and n % 2 == 0 and 2 * (head_count // parts) == n


def solution(mesh):
    def step(*args):
        body = local if fits(mesh, args[3].shape[0]) else local_general
        return sharded(mesh, body)(*args)

    return step


def sharded(mesh, body):
    return jax.shard_map(
        body,
        mesh=mesh,
        in_specs=(
            P("ep", "tp"),
            P("ep", "tp"),
            P("ep", "tp"),
            P("tp"),
            P(),
            P("ep", None),
            P(),
            P("ep", None),
            P("ep", None),
            P("ep", None, "tp"),
            P("ep", None, "tp"),
            P("ep", "tp", None),
        ),
        out_specs=(P("ep", "tp"), P("ep", "tp")),
        check_vma=False,
    )
```
